32 devices in a mesh: sp: 8 (over z, x), tp: 4 (over y, core).
Axes of the slice: x: 2, y: 2, z: 4, core: 2. Of those that a mesh axis runs over, the one named last changes fastest.
Arguments:
- stream: bfloat16 [4096, 2048], P(('sp', 'tp')), may hold values from -6 to 6
- pool_in: bfloat16 [4096, 1024], P('sp', 'tp'), may hold values from -6 to 6
- doc_ids: int32 [4096], P('sp'), may hold values from 0 to 7, never falling along the last dimension, each value on 1 to 1024 neighbouring positions
- pool_map: bfloat16 [4, 256, 512], P('tp'), may hold values from -0.375 to 0.375
- pool_scale: float32 [2048], P('tp'), may hold values from 0.1 to 1.9
- out_weight: bfloat16 [2048, 2048], P('tp'), may hold values from -0.125 to 0.125
- norm_gain: float32 [2048], replicated, may hold values from 0.1 to 1.9
- routes: int32 [4096, 2], P('sp'), may hold values from 0 to 7, all different within a row; in each aligned block of 128 rows (0 to 127, 128 to 255, ...) at most 48 rows name the same one
- route_weight: float32 [4096, 2], P(('sp', 'tp')), may hold values from 0.2 to 1
- expert_gate: bfloat16 [8, 2048, 1024], P('sp', None, 'tp'), may hold values from -0.125 to 0.125
- expert_up: bfloat16 [8, 2048, 1024], P('sp', None, 'tp'), may hold values from -0.125 to 0.125
- expert_down: bfloat16 [8, 1024, 2048], P('sp', 'tp'), may hold values from -0.1875 to 0.1875
Outputs:
- result: bfloat16 [4096, 2048], P(('sp', 'tp'))
The draws below stay inside these ranges and needn't reach their ends.
Inputs may be any that keep to these rules, and one draw needn't show every extreme that they name: `routes`: each token names 2 different experts; in each aligned block of 128 rows no expert is named by more than 48 rows, a bound that some block reaches. `doc_ids`: never falling; each document holds at most 1024 positions.
All inputs are finite; a program needn't handle non-finite values.
Results may differ from the reference program's by a relative error of at most 0.014.
Values may be sent and summed in bfloat16 or wider, within the bound.
A program may use at most 64 MiB of HBM per device.

```python
import math
import jax
import jax.numpy as jnp
import numpy as np
from jax import lax

D = 2048
PW = 1024
GROUPS = 4
FF = 1024
TOPK = 2
DOC_COUNT = 8
GW = 256
GOUT = 512
QUART = 128
TOKENS = 4096
EXPERTS = 8
CAP = 48
FF_PART = 256
DOC_MOST = 1024
N_TP = 4


def block_levels(rng, dims, cuts, low, high):
    loudness, own = 1.0, jax.random.fold_in(rng, 6)
    for dim, blocks in cuts:
        heights = jnp.exp(jax.random.uniform(jax.random.fold_in(own, dim), (blocks,), jnp.float32, low / len(cuts), high / len(cuts)))
        loudness = loudness * jnp.repeat(heights, dims[dim] // blocks).reshape([-1 if axis == dim else 1 for axis in range(len(dims))])
    return loudness


def split_up(number_of, total, bound, lean):
    loads = [(1 << 20) // math.isqrt(rank ** lean) + 1 for rank in range(2, number_of + 1)]
    spare, holding = total - bound - (number_of - 1), [1] * (number_of - 1)
    while spare > 0:
        candidates = [i for i in range(number_of - 1) if holding[i] < bound]
        pool, budget = sum([loads[i] for i in candidates]), spare
        for i in candidates:
            addition = min(bound - holding[i], max(1, budget * loads[i] // pool), spare)
            holding[i] = holding[i] + addition
            spare = spare - addition
    return np.array([bound] + holding)


def ragged_sizes(stream_key, number_of, total, reach, lean):
    if number_of == 2:
        one = jax.random.randint(stream_key, (), max(1, total - reach), min(reach, total - 1) + 1)
        return jnp.stack([one, total - one])
    lengths = jnp.asarray(split_up(number_of, total, reach, lean), jnp.int32)
    twos = (number_of - 1) // 2
    donor, receiver = lengths[1:1 + 2 * twos:2], lengths[2:2 + 2 * twos:2]
    slack = jnp.minimum(donor - 1, reach - receiver)
    passed = jax.random.randint(jax.random.fold_in(stream_key, 1), (twos,), 0, 1 << 20) % (slack + 1)
    lengths = lengths.at[1:1 + 2 * twos:2].set(donor - passed).at[2:2 + 2 * twos:2].set(receiver + passed)
    return lengths[jax.random.permutation(jax.random.fold_in(stream_key, 2), number_of)]


def routed_block(rng, own, number, rows, number_of, top, most, skew):
    order = jax.random.permutation(rng, number_of)
    heavy_load, usual = shares(number_of, rows * top, most, skew, True), shares(number_of, rows * top, most, skew, False)
    places = jnp.arange(number_of)

    def named(tallies, rotation):
        used = int((tallies > 0).sum())
        fixed = max(1, used // 4)
        moved = fixed + (places - fixed + rotation * (used - fixed)) % max(1, number_of - fixed)
        return jnp.zeros((number_of,), jnp.int32).at[order[jnp.where(places < fixed, places, moved)]].set(jnp.asarray(tallies, jnp.int32))

    tallies = jnp.where(number % 4 == 0, named(heavy_load, number // 4), named(usual, number - number // 4 - 1))
    mixed = jax.random.permutation(jax.random.fold_in(own, 3), number_of)
    giver, sink = mixed[0:number_of // 2 * 2:2], mixed[1:number_of // 2 * 2:2]
    margin = jnp.minimum(tallies[giver] - 1, most - tallies[sink]) // 2
    margin = jnp.where((giver == order[0]) | (sink == order[0]) | (tallies[sink] == 0), 0, jnp.maximum(margin, 0))
    moved = jax.random.randint(jax.random.fold_in(own, 4), (number_of // 2,), 0, 1 << 20) % (margin + 1)
    tallies = tallies.at[giver].add(-moved).at[sink].add(moved)
    items = jnp.searchsorted(jnp.cumsum(tallies), jnp.arange(rows * top), side="right").astype(jnp.int32)
    grid = items.reshape(top, rows).T
    grid = grid[jax.random.permutation(jax.random.fold_in(own, 1), rows)]
    rotation = jax.random.randint(jax.random.fold_in(own, 2), (rows, 1), 0, top)
    return jnp.take_along_axis(grid, (jnp.arange(top)[None, :] + rotation) % top, axis=1)


def shares(number_of, total, bound, skew, full):
    portions = [(1 << 20) // math.isqrt(grade ** skew) + 1 for grade in range(1, number_of + 1)]
    largest = bound if full else min(bound, max(-(-total // number_of), total * portions[0] // sum(portions)))
    least = 1 if total - largest >= number_of - 1 else 0
    given, rest = [largest] + [least] * (number_of - 1), total - largest - least * (number_of - 1)
    while rest > 0:
        movable = [i for i in range(1, number_of) if given[i] < largest] or [i for i in range(1, number_of) if given[i] < bound]
        whole, left = sum([portions[i] for i in movable]), rest
        for i in movable:
            more = min(bound - given[i], max(1, left * portions[i] // whole), rest)
            given[i] = given[i] + more
            rest = rest - more
    return np.array(given)


def normal_values(stream_key, shape, width, limit, pieces=(), kind=jnp.bfloat16):
    drawn = width * jax.random.normal(stream_key, shape, jnp.float32)
    if pieces:
        drawn = drawn * block_levels(stream_key, shape, pieces, -0.22, 0.18)
    return jnp.clip(drawn, -limit, limit).astype(kind)


def setup_inputs(seed: int = 0) -> dict:
    streams_of = jax.random.split(jax.random.key(seed), 13)
    stream = normal_values(streams_of[0], (TOKENS, D), 1.0, 6.0, ((0, 32),))
    pool_in = normal_values(streams_of[1], (TOKENS, PW), 1.0, 6.0, ((0, 8), (1, 4)))
    doc_ids = jnp.searchsorted(jnp.cumsum(ragged_sizes(streams_of[2], DOC_COUNT, TOKENS, DOC_MOST, 1)), jnp.arange(TOKENS), side="right").astype(jnp.int32)
    pool_map = normal_values(streams_of[3], (GROUPS, GW, GOUT), GW ** -0.5, 0.375, ((0, 4),))
    pool_scale = jnp.clip(1.0 + 0.18 * jax.random.normal(streams_of[4], (D,), jnp.float32), 0.1, 1.9)
    out_weight = normal_values(streams_of[5], (D, D), D ** -0.5, 0.125, ((0, 4),))
    norm_gain = jnp.clip(1.0 + 0.18 * jax.random.normal(streams_of[6], (D,), jnp.float32), 0.1, 1.9)
    routes_keys = jax.random.split(jax.random.fold_in(streams_of[7], 1), TOKENS // QUART)
    routes_turns = jax.random.permutation(jax.random.fold_in(streams_of[7], 3), TOKENS // QUART)
    routes = jax.vmap(lambda own, number: routed_block(jax.random.fold_in(streams_of[7], 2), own, number, QUART, EXPERTS, TOPK, CAP, 1))(routes_keys, routes_turns).reshape((TOKENS, TOPK))
    route_weight = jnp.clip(0.2 + 0.8 * jax.random.uniform(streams_of[8], (TOKENS, TOPK), jnp.float32) ** block_levels(streams_of[8], (TOKENS, TOPK), ((0, 32),), -0.2, 0.2), 0.2, 1.0)
    expert_gate = normal_values(streams_of[9], (EXPERTS, D, FF), D ** -0.5, 0.125, ((0, 8), (2, 4)))
    expert_up = normal_values(streams_of[10], (EXPERTS, D, FF), D ** -0.5, 0.125, ((0, 8), (2, 4)))
    expert_down = normal_values(streams_of[11], (EXPERTS, FF, D), FF ** -0.5, 0.1875, ((0, 8), (1, 4)))
    return dict(stream=stream, pool_in=pool_in, doc_ids=doc_ids, pool_map=pool_map, pool_scale=pool_scale, out_weight=out_weight, norm_gain=norm_gain, routes=routes, route_weight=route_weight, expert_gate=expert_gate, expert_up=expert_up, expert_down=expert_down)


EPS = 1e-06

def reference(stream, pool_in, doc_ids, pool_map, pool_scale, out_weight, norm_gain, routes, route_weight, expert_gate, expert_up, expert_down):
    total_rows = pool_in.shape[0]
    positions = jnp.arange(total_rows, dtype=jnp.int32)
    starts_here = jnp.concatenate([jnp.ones((1,), jnp.bool_), doc_ids[1:] != doc_ids[:-1]])
    doc_start = lax.cummax(jnp.where(starts_here, positions, 0).astype(jnp.int32), axis=0)
    source_rows = pool_in.astype(jnp.float32)
    branch_parts = []
    for group_index in range(GROUPS):
        window = 2 << group_index
        group_cols = source_rows[:, group_index * GW:(group_index + 1) * GW]
        running = jnp.zeros_like(group_cols)
        counts = jnp.zeros((total_rows,), jnp.float32)
        for offset in range(window):
            shifted = jnp.concatenate([jnp.zeros((offset, GW), jnp.float32), group_cols[:total_rows - offset]], axis=0)
            in_window = positions - offset >= doc_start
            running = running + jnp.where(in_window[:, None], shifted, 0.0)
            counts = counts + in_window.astype(jnp.float32)
        pooled = (running / counts[:, None] - group_cols).astype(jnp.bfloat16)
        mapped = jnp.dot(pooled, pool_map[group_index], preferred_element_type=jnp.float32)
        branch_parts.append((mapped * pool_scale[group_index * GOUT:(group_index + 1) * GOUT]).astype(jnp.bfloat16))
    branch = jnp.concatenate(branch_parts, axis=1)
    mixed_rows = (stream.astype(jnp.float32) + jnp.dot(branch, out_weight, preferred_element_type=jnp.float32)).astype(jnp.bfloat16)
    mixed_up = mixed_rows.astype(jnp.float32)
    normed = (mixed_up * lax.rsqrt(lax.optimization_barrier(jnp.mean(mixed_up * mixed_up, axis=1, keepdims=True)) + EPS) * norm_gain).astype(jnp.bfloat16)
    block_count = total_rows // QUART
    flattened = routes.reshape(-1).astype(jnp.int32)
    one_hot = (flattened[:, None] == jnp.arange(EXPERTS, dtype=jnp.int32)[None, :]).astype(jnp.int32)
    blocked = one_hot.reshape(block_count, QUART * TOPK, EXPERTS)
    ranking = lax.optimization_barrier(jnp.sum((jnp.cumsum(blocked, axis=1) - blocked) * blocked, axis=2)).reshape(-1).astype(jnp.int32)
    assign_ids = jnp.arange(total_rows * TOPK, dtype=jnp.int32)
    block_ids = (assign_ids // (QUART * TOPK)).astype(jnp.int32)
    target_slot = ((flattened * block_count + block_ids) * CAP + ranking).astype(jnp.int32)
    per_expert = block_count * CAP
    slot_token = jnp.zeros((EXPERTS * per_expert,), jnp.int32).at[target_slot].set((assign_ids // TOPK).astype(jnp.int32))
    slot_weight = jnp.zeros((EXPERTS * per_expert,), jnp.float32).at[target_slot].set(route_weight.reshape(-1))

    def one_expert(accumulated, expert_index):
        begin_slot = (expert_index * per_expert).astype(jnp.int32)
        tokens_here = lax.dynamic_slice_in_dim(slot_token, begin_slot, per_expert)
        weights_here = lax.dynamic_slice_in_dim(slot_weight, begin_slot, per_expert)
        inputs = normed[tokens_here]
        gate_pre = jnp.dot(inputs, expert_gate[expert_index], preferred_element_type=jnp.float32)
        up_pre = jnp.dot(inputs, expert_up[expert_index], preferred_element_type=jnp.float32)
        hidden = (jax.nn.silu(gate_pre) * up_pre).astype(jnp.bfloat16)
        down_rows = expert_down[expert_index]
        summed = jnp.zeros((per_expert, D), jnp.float32)
        for part_index in range(N_TP):
            part_begin = part_index * FF_PART
            part_out = jnp.dot(hidden[:, part_begin:part_begin + FF_PART], down_rows[part_begin:part_begin + FF_PART], preferred_element_type=jnp.float32).astype(jnp.bfloat16)
            summed = summed + lax.optimization_barrier(part_out).astype(jnp.float32)
        expert_out = lax.optimization_barrier(summed.astype(jnp.bfloat16)).astype(jnp.float32)
        return (accumulated.at[tokens_here].add(weights_here[:, None] * expert_out), None)
    accumulated, unused_out = lax.scan(one_expert, jnp.zeros((total_rows, D), jnp.float32), jnp.arange(EXPERTS, dtype=jnp.int32))
    return (mixed_up + accumulated).astype(jnp.bfloat16)
```

```python
import functools

import jax
import jax.numpy as jnp
from jax import lax
from jax.experimental import pallas as pl
from jax.experimental.pallas import tpu as pltpu
from jax.sharding import PartitionSpec as P

HALO = 16
COLS = 512
PIECE = 256
EPS = 1e-06
MESH = pl.DeviceIdType.MESH
F32 = jnp.float32
BF16 = jnp.bfloat16


def flipped(index, mask):
    bit = 1
    while bit <= mask:
        if mask & bit:
            index = index + bit - 2 * bit * (index // bit % 2)
        bit *= 2
    return index


def window_sums(prior, prior_docs, own, own_docs, window):
    width = own.shape[1]
    ext_docs = jnp.concatenate([prior_docs, own_docs], axis=0)
    total = jnp.concatenate([prior, own], axis=0)
    counts = jnp.ones(ext_docs.shape, F32)
    step = 1
    while step < HALO:
        keep = (pltpu.roll(ext_docs, step, 0) == ext_docs) & (step < window)
        counts = counts + jnp.where(keep, pltpu.roll(counts, step, 0), 0.0)
        keep_wide = jnp.concatenate([keep.astype(F32)] * (width // 128), axis=1) > 0.5
        total = total + jnp.where(keep_wide, pltpu.roll(total, step, 0), 0.0)
        step *= 2
    counts_wide = jnp.concatenate([counts] * (width // 128), axis=1)
    return (total[HALO:] / counts_wide[HALO:] - own).astype(BF16)


def kernel(
    n_sp, n_tp, quarter, capacity, top,
    stream, pool_in, docs_row, pool_map, pool_scale, out_weight, gain, routes, weights,
    gate, up, down,
    out,
    gates, ups, downs, outw, halo, halo_docs, branch, partial, pair_send, pair_recv,
    far_send, far_recv, mixed, dispatch, arrived, crossed, hidden, hidden_send,
    answers, returned, docs,
    local_sem, halo_ssem, halo_rsem, g_ssem, g_rsem, w_ssem, w_rsem, n_ssem, f_ssem,
    p_ssem, p_rsem, y_ssem, y_rsem, d_ssem, d_rsem, c_ssem, c_rsem, h_ssem, h_rsem,
    r_ssem, r_rsem,
):
    sp, tp = lax.axis_index("sp"), lax.axis_index("tp")
    n_chip = n_tp // 2
    chip, parity = tp // 2, tp % 2
    other = 1 - parity
    partner = chip * 2 + other
    rows = pool_in.shape[0]
    width = stream.shape[1]
    ff = gate.shape[1]
    slots = n_sp * capacity
    half = n_sp // 2
    team, member = sp // half, sp % half
    span = half // 2
    chunks = width // COLS
    pieces = width // PIECE
    others = range(1, n_chip)

    def same(m):
        return (chip + m) % n_chip * 2 + parity

    def remote(src, dst, ssem, rsem, to):
        return pltpu.make_async_remote_copy(
            src_ref=src, dst_ref=dst, send_sem=ssem, recv_sem=rsem,
            device_id=to, device_id_type=MESH,
        )

    def peer(at):
        if at < half:
            return (1 - team) * half + flipped(member, at)
        return team * half + flipped(member, at - half)

    def cols(c):
        return pl.ds(c * COLS, COLS)

    def wide(p):
        return pl.ds(p * PIECE, PIECE)

    def block(e):
        return pl.ds(pl.multiple_of(e * capacity, 16), capacity)

    def owned(q):
        return pl.ds(pl.multiple_of(q * quarter, quarter), quarter)

    own_copies = [
        pltpu.make_async_copy(out_weight, outw, local_sem.at[0]),
        pltpu.make_async_copy(gate, gates.at[:, pl.ds(0, ff)], local_sem.at[1]),
        pltpu.make_async_copy(up, ups.at[:, pl.ds(0, ff)], local_sem.at[2]),
        pltpu.make_async_copy(down, downs.at[pl.ds(0, ff)], local_sem.at[3]),
    ]
    for c in own_copies:
        c.start()

    barrier = pltpu.get_barrier_semaphore()
    for d in range(1, n_sp):
        pl.semaphore_signal(barrier, inc=1, device_id=((sp + d) % n_sp, tp), device_id_type=MESH)
    pl.semaphore_signal(barrier, inc=1, device_id=(sp, partner), device_id_type=MESH)
    for m in others:
        pl.semaphore_signal(barrier, inc=1, device_id=(sp, same(m)), device_id_type=MESH)

    docs[...] = jnp.transpose(jnp.broadcast_to(docs_row[...].astype(F32), (128, rows)))
    window = jnp.left_shift(jnp.int32(2), tp)
    group_width = pool_in.shape[1]
    pooled = window_sums(
        jnp.zeros((HALO, group_width), F32), jnp.full((HALO, 128), -1.0, F32),
        pool_in[...].astype(F32), docs[...], window,
    )
    branch[...] = (
        jnp.dot(pooled, pool_map[...], preferred_element_type=F32) * pool_scale[...]
    ).astype(BF16)
    own_copies[0].wait()
    for c in range(chunks):
        partial[:, cols(c)] = jnp.dot(branch[...], outw[:, cols(c)], preferred_element_type=F32)

    def pair_owner(m):
        return (chip + m) % n_chip * 2 + other

    for m in range(n_chip):
        pair_send[m] = partial[owned(pair_owner(m)), :].astype(BF16)

    names = lax.broadcasted_iota(jnp.int32, (128, quarter), 0)
    own_routes = routes[:, owned(tp)]
    hots = [(own_routes[k : k + 1, :] == names).astype(F32) for k in range(top)]
    named = functools.reduce(lambda a, b: a + b, hots)
    above = (
        lax.broadcasted_iota(jnp.int32, (quarter, quarter), 0)
        < lax.broadcasted_iota(jnp.int32, (quarter, quarter), 1)
    ).astype(BF16)
    before = jnp.dot(named.astype(BF16), above, preferred_element_type=F32)
    slot_names = lax.broadcasted_iota(jnp.int32, (slots, quarter), 0)
    places = []
    for k in range(top):
        rank = jnp.sum(hots[k] * before, axis=0, keepdims=True).astype(jnp.int32)
        places.append((slot_names == own_routes[k : k + 1, :] * capacity + rank).astype(F32))
    spread = functools.reduce(lambda a, b: a + b, places).astype(BF16)
    picks = [jnp.transpose(p).astype(BF16) for p in places]
    scales = [
        jnp.transpose(jnp.broadcast_to(weights[k : k + 1, :], (128, quarter)))[:, :1]
        for k in range(top)
    ]

    pl.semaphore_wait(barrier, n_sp - 1 + 1 + n_chip - 1)

    right = ((sp + 1) % n_sp, tp)
    halo_copies = [
        remote(pool_in.at[pl.ds(rows - HALO, HALO)], halo, halo_ssem.at[0], halo_rsem.at[0], right),
        remote(docs.at[pl.ds(rows - HALO, HALO)], halo_docs, halo_ssem.at[1], halo_rsem.at[1], right),
    ]
    for c in halo_copies:
        c.start()

    def far_down(p, m):
        j = (n_chip - m) % n_chip
        return remote(
            down.at[:, wide(p)], downs.at[pl.ds(2 * j * ff, ff), wide(p)],
            w_ssem.at[m, p], w_rsem.at[2 * j, p], (sp, same(m)),
        )

    def near_down(p):
        return remote(
            down.at[:, wide(p)], downs.at[pl.ds(ff, ff), wide(p)],
            n_ssem.at[p], w_rsem.at[1, p], (sp, partner),
        )

    def forward_down(p, m):
        return remote(
            downs.at[pl.ds(2 * m * ff, ff), wide(p)],
            downs.at[pl.ds((2 * m + 1) * ff, ff), wide(p)],
            f_ssem.at[m, p], w_rsem.at[2 * m + 1, p], (sp, partner),
        )

    near_hidden = [
        remote(gate, gates.at[:, pl.ds(ff, ff)], g_ssem.at[0], g_rsem.at[0], (sp, partner)),
        remote(up, ups.at[:, pl.ds(ff, ff)], g_ssem.at[1], g_rsem.at[1], (sp, partner)),
    ]

    def send_down(*which):
        for p in which:
            for m in others:
                far_down(p, m).start()

    def pair_copy(m, c):
        return remote(
            pair_send.at[m, :, cols(c)], pair_recv.at[m, :, cols(c)],
            p_ssem.at[m, c], p_rsem.at[m, c], (sp, partner),
        )

    order = list(others) + [0]
    send_down(0)
    for m in order:
        @pl.when(pair_owner(m) != 0)
        def _(m=m):
            for c in range(chunks):
                pair_copy(m, c).start()

    for c in halo_copies:
        c.wait_recv()
    first = sp == 0
    head = window_sums(
        jnp.where(first, 0.0, halo[...].astype(F32)), jnp.where(first, -1.0, halo_docs[...]),
        pool_in[pl.ds(0, HALO), :].astype(F32), docs[pl.ds(0, HALO), :], window,
    )
    head = (jnp.dot(head, pool_map[...], preferred_element_type=F32) * pool_scale[...]).astype(BF16)
    head = jnp.dot(head, outw[...], preferred_element_type=F32)
    partial[pl.ds(0, HALO), :] = head
    for m in order:
        @pl.when(pair_owner(m) == 0)
        def _(m=m):
            pair_send[m, pl.ds(0, HALO), :] = head.astype(BF16)
            for c in range(chunks):
                pair_copy(m, c).start()

    def far_copy(m, c):
        j = (n_chip - m) % n_chip
        return remote(
            far_send.at[m, :, cols(c)], far_recv.at[j, :, cols(c)],
            y_ssem.at[m, c], y_rsem.at[j, c], (sp, same(m)),
        )

    for m in others:
        for c in range(chunks):
            pair_copy(m, c).wait_recv()
            far_send[m, :, cols(c)] = (
                partial[owned(same(m)), cols(c)] + pair_recv[m, :, cols(c)].astype(F32)
            ).astype(BF16)
            far_copy(m, c).start()
    for c in near_hidden:
        c.start()
    for p in range(pieces):
        near_down(p).start()
    send_down(1, 2)

    everything = pl.ds(0, width)

    def outward(at, c=None):
        e = peer(at)
        columns = everything if c is None else cols(c)
        slot = c or 0
        return remote(
            dispatch.at[block(e), columns], arrived.at[pl.ds(at * capacity, capacity), columns],
            d_ssem.at[at, slot], d_rsem.at[at, slot], (e, tp),
        )

    for c in range(chunks):
        pair_copy(0, c).wait_recv()
        mine = partial[owned(tp), cols(c)] + pair_recv[0, :, cols(c)].astype(F32)
        for m in others:
            far_copy((n_chip - m) % n_chip, c).wait_recv()
            mine = mine + far_recv[m, :, cols(c)].astype(F32)
        mixed[:, cols(c)] = (stream[:, cols(c)].astype(F32) + mine).astype(BF16)
        dispatch[:, cols(c)] = jnp.dot(
            spread, mixed[:, cols(c)], preferred_element_type=F32
        ).astype(BF16)
        for at in range(span):
            outward(at, c).start()
    for at in list(range(half + 1, half + span)) + list(range(span, half)) + list(
        range(half + span, n_sp)
    ):
        outward(at).start()
    arrived[pl.ds(half * capacity, capacity), :] = dispatch[block(sp), :]

    size = span * capacity

    def places_of(g):
        return range(g * span, (g + 1) * span)

    def lines(g):
        return pl.ds(g * size, size)

    def gated(x):
        g = jnp.dot(x, gates[...], preferred_element_type=F32)
        u = jnp.dot(x, ups[...], preferred_element_type=F32)
        return (g / (1.0 + jnp.exp(-g)) * u).astype(BF16)

    def cross_copy(m, g):
        j = (n_chip - m) % n_chip
        return remote(
            crossed.at[0, lines(g)], crossed.at[j, lines(g)],
            c_ssem.at[m, g], c_rsem.at[j, g], (sp, same(m)),
        )

    def hidden_copy(j, g):
        m = (n_chip - j) % n_chip
        return remote(
            hidden_send.at[j - 1, lines(g)], hidden.at[lines(g), pl.ds(2 * m * ff, 2 * ff)],
            h_ssem.at[j, g], h_rsem.at[m, g], (sp, same(j)),
        )

    def normalize(g):
        for at in places_of(g):
            if at < span:
                for c in range(chunks):
                    outward(at, c).wait_recv()
            elif at != half:
                outward(at).wait_recv()
        value = arrived[lines(g), :].astype(F32)
        crossed[0, lines(g), :] = (
            value * lax.rsqrt(jnp.mean(value * value, axis=1, keepdims=True) + EPS) * gain[...]
        ).astype(BF16)
        for m in others:
            cross_copy(m, g).start()

    ready = []

    def own_hidden(g):
        if not ready:
            ready.append(True)
            for c in own_copies[1:3]:
                c.wait()
            for c in near_hidden:
                c.wait_recv()
        hidden[lines(g), pl.ds(0, 2 * ff)] = gated(crossed[0, lines(g), :])

    def far_hidden(g):
        for j in others:
            cross_copy((n_chip - j) % n_chip, g).wait_recv()
            hidden_send[j - 1, lines(g), :] = gated(crossed[j, lines(g), :])
            hidden_copy(j, g).start()

    held = set()

    def pass_down(*which):
        for p in which:
            for m in others:
                j = (n_chip - m) % n_chip
                far_down(p, j).wait_recv()
                forward_down(p, m).start()

    def homeward(at, p):
        e = peer(at)
        return remote(
            answers.at[pl.ds(at * capacity, capacity), wide(p)], returned.at[block(sp), wide(p)],
            r_ssem.at[at, p], r_rsem.at[at, p], (e, tp),
        )

    def answer(g, *which):
        if ("hidden", g) not in held:
            held.add(("hidden", g))
            for m in others:
                hidden_copy((n_chip - m) % n_chip, g).wait_recv()
        for p in which:
            if p not in held:
                if not held & set(range(pieces)):
                    own_copies[3].wait()
                held.add(p)
                near_down(p).wait_recv()
                for m in others:
                    forward_down(p, m).wait_recv()
            answers[lines(g), wide(p)] = jnp.dot(
                hidden[lines(g), :], downs[:, wide(p)], preferred_element_type=F32
            ).astype(BF16)
            for at in places_of(g):
                if at == half:
                    returned[block(sp), wide(p)] = answers[pl.ds(at * capacity, capacity), wide(p)]
                else:
                    homeward(at, p).start()

    early = tuple(range(pieces - 3))
    late = tuple(range(pieces - 3, pieces))
    normalize(2)
    own_hidden(2)
    normalize(0)
    send_down(*early[3:])
    own_hidden(0)
    far_hidden(2)
    far_hidden(0)
    send_down(late[0])
    pass_down(*early)
    answer(0, *early)
    normalize(1)
    send_down(*late[1:])
    own_hidden(1)
    answer(2, *early)
    far_hidden(1)
    normalize(3)
    own_hidden(3)
    pass_down(*late)
    answer(1, *early)
    answer(0, *late)
    answer(1, *late)
    answer(2, *late)
    far_hidden(3)
    answer(3, *range(pieces))

    for p in range(pieces):
        for at in range(n_sp):
            if at != half:
                homeward(at, p).wait_recv()
        result = mixed[:, wide(p)].astype(F32)
        for k in range(top):
            result = result + scales[k] * jnp.dot(
                picks[k], returned[:, wide(p)], preferred_element_type=F32
            )
        out[:, wide(p)] = result.astype(BF16)

    for c in halo_copies + near_hidden:
        c.wait_send()
    for m in range(n_chip):
        for c in range(chunks):
            pair_copy(m, c).wait_send()
    for p in range(pieces):
        near_down(p).wait_send()
        for m in others:
            far_down(p, m).wait_send()
            forward_down(p, m).wait_send()
    for m in others:
        for c in range(chunks):
            far_copy(m, c).wait_send()
        for g in range(4):
            cross_copy(m, g).wait_send()
            hidden_copy(m, g).wait_send()
    for at in range(n_sp):
        if at == half:
            continue
        if at < span:
            for c in range(chunks):
                outward(at, c).wait_send()
        else:
            outward(at).wait_send()
        for p in range(pieces):
            homeward(at, p).wait_send()


def per_device(
    n_sp, n_tp,
    stream, pool_in, doc_ids, pool_map, pool_scale, out_weight, norm_gain, routes, route_weight,
    expert_gate, expert_up, expert_down,
):
    rows, group_width = pool_in.shape
    quarter, width = stream.shape
    top = routes.shape[1]
    ff = expert_gate.shape[2]
    capacity = max(2, 3 * top * quarter // (2 * n_sp))
    capacity = -(-capacity // 16) * 16
    slots = n_sp * capacity
    n_chip = n_tp // 2
    vmem = pl.BlockSpec(memory_space=pltpu.VMEM)
    hbm = pl.BlockSpec(memory_space=pl.ANY)
    dma = pltpu.SemaphoreType.DMA
    V = pltpu.VMEM
    branch_width = out_weight.shape[0]
    chunks = width // COLS
    pieces = width // PIECE
    return pl.pallas_call(
        functools.partial(kernel, n_sp, n_tp, quarter, capacity, top),
        out_shape=jax.ShapeDtypeStruct((quarter, width), BF16),
        in_specs=[vmem] * 5 + [hbm] + [vmem] * 3 + [hbm] * 3,
        out_specs=vmem,
        scratch_shapes=[
            V((width, 2 * ff), BF16),
            V((width, 2 * ff), BF16),
            V((n_tp * ff, width), BF16),
            V((branch_width, width), BF16),
            V((HALO, group_width), BF16),
            V((HALO, 128), F32),
            V((rows, branch_width), BF16),
            V((rows, width), F32),
            V((n_chip, quarter, width), BF16),
            V((n_chip, quarter, width), BF16),
            V((n_chip, quarter, width), BF16),
            V((n_chip, quarter, width), BF16),
            V((quarter, width), BF16),
            V((slots, width), BF16),
            V((slots, width), BF16),
            V((n_chip, slots, width), BF16),
            V((slots, n_tp * ff), BF16),
            V((n_chip - 1, slots, 2 * ff), BF16),
            V((slots, width), BF16),
            V((slots, width), BF16),
            V((rows, 128), F32),
            dma((4,)),
            dma((2,)),
            dma((2,)),
            dma((2,)),
            dma((2,)),
            dma((n_chip, pieces)),
            dma((n_tp, pieces)),
            dma((pieces,)),
            dma((n_chip, pieces)),
            dma((n_chip, chunks)),
            dma((n_chip, chunks)),
            dma((n_chip, chunks)),
            dma((n_chip, chunks)),
            dma((n_sp, chunks)),
            dma((n_sp, chunks)),
            dma((n_chip, 4)),
            dma((n_chip, 4)),
            dma((n_chip, 4)),
            dma((n_chip, 4)),
            dma((n_sp, pieces)),
            dma((n_sp, pieces)),
        ],
        compiler_params=pltpu.CompilerParams(
            collective_id=0, has_side_effects=True, vmem_limit_bytes=60 * 1024 * 1024
        ),
    )(
        stream, pool_in, doc_ids[None, :], pool_map[0],
        pool_scale[None, :], out_weight, norm_gain[None, :], routes.T, route_weight.T,
        expert_gate[0], expert_up[0], expert_down[0],
    )


def solution(mesh):
    in_specs = (
        P(("sp", "tp"), None),
        P("sp", "tp"),
        P("sp"),
        P("tp", None, None),
        P("tp"),
        P("tp", None),
        P(),
        P("sp", None),
        P(("sp", "tp"), None),
        P("sp", None, "tp"),
        P("sp", None, "tp"),
        P("sp", "tp", None),
    )
    out_specs = P(("sp", "tp"), None)
    return jax.shard_map(
        functools.partial(per_device, mesh.shape["sp"], mesh.shape["tp"]),
        mesh=mesh, in_specs=in_specs, out_specs=out_specs, check_vma=False,
    )
```

```python
import functools

import jax
import jax.numpy as jnp
from jax import lax
from jax.experimental import pallas as pl
from jax.experimental.pallas import tpu as pltpu
from jax.sharding import PartitionSpec as P

HALO = 16
COLS = 512
PIECE = 256
EPS = 1e-06
MESH = pl.DeviceIdType.MESH
F32 = jnp.float32
BF16 = jnp.bfloat16


def flipped(index, mask):
    bit = 1
    while bit <= mask:
        if mask & bit:
            index = index + bit - 2 * bit * (index // bit % 2)
        bit *= 2
    return index


def window_sums(prior, prior_docs, own, own_docs, window):
    width = own.shape[1]
    ext_docs = jnp.concatenate([prior_docs, own_docs], axis=0)
    total = jnp.concatenate([prior, own], axis=0)
    counts = jnp.ones(ext_docs.shape, F32)
    step = 1
    while step < HALO:
        keep = (pltpu.roll(ext_docs, step, 0) == ext_docs) & (step < window)
        counts = counts + jnp.where(keep, pltpu.roll(counts, step, 0), 0.0)
        keep_wide = jnp.concatenate([keep.astype(F32)] * (width // 128), axis=1) > 0.5
        total = total + jnp.where(keep_wide, pltpu.roll(total, step, 0), 0.0)
        step *= 2
    counts_wide = jnp.concatenate([counts] * (width // 128), axis=1)
    return (total[HALO:] / counts_wide[HALO:] - own).astype(BF16)


def kernel(
    n_sp, n_tp, quarter, capacity, top,
    stream, pool_in, docs_row, pool_map, pool_scale, out_weight, gain, routes, weights,
    gate, up, down,
    out,
    gates, ups, downs, outw, halo, halo_docs, branch, partial, pair_send, pair_recv,
    far_send, far_recv, mixed, dispatch, arrived, crossed, hidden, hidden_send,
    answers, returned, mixed_sib, dispatch_sib, docs, map_here, stream_here, out_here,
    local_sem, halo_ssem, halo_rsem, g_ssem, g_rsem, w_ssem, w_rsem, n_ssem, f_ssem,
    p_ssem, p_rsem, y_ssem, y_rsem, d_ssem, d_rsem, c_ssem, c_rsem, h_ssem, h_rsem,
    r_ssem, r_rsem, out_sem, a_ssem, a_rsem, s_ssem, s_rsem,
):
    sp, tp = lax.axis_index("sp"), lax.axis_index("tp")
    n_chip = n_tp // 2
    chip, parity = tp // 2, tp % 2
    other = 1 - parity
    partner = chip * 2 + other
    rows = pool_in.shape[0]
    width = stream.shape[1]
    ff = gate.shape[1]
    slots = n_sp * capacity
    half = n_sp // 2
    team, member = sp // half, sp % half
    span = half // 2
    chunks = width // COLS
    pieces = width // PIECE
    others = range(1, n_chip)

    def same(m):
        return (chip + m) % n_chip * 2 + parity

    def remote(src, dst, ssem, rsem, to):
        return pltpu.make_async_remote_copy(
            src_ref=src, dst_ref=dst, send_sem=ssem, recv_sem=rsem,
            device_id=to, device_id_type=MESH,
        )

    def peer(at):
        if at < half:
            return (1 - team) * half + flipped(member, at)
        return team * half + flipped(member, at - half)

    def cols(c):
        return pl.ds(c * COLS, COLS)

    def wide(p):
        return pl.ds(p * PIECE, PIECE)

    def block(e):
        return pl.ds(pl.multiple_of(e * capacity, 16), capacity)

    def owned(q):
        return pl.ds(pl.multiple_of(q * quarter, quarter), quarter)

    barrier = pltpu.get_barrier_semaphore()
    for d in range(1, n_sp):
        pl.semaphore_signal(barrier, inc=1, device_id=((sp + d) % n_sp, tp), device_id_type=MESH)
    pl.semaphore_signal(barrier, inc=1, device_id=(sp, partner), device_id_type=MESH)
    for m in others:
        pl.semaphore_signal(barrier, inc=1, device_id=(sp, same(m)), device_id_type=MESH)

    own_copies = [
        pltpu.make_async_copy(out_weight, outw, local_sem.at[0]),
        pltpu.make_async_copy(gate, gates.at[:, pl.ds(0, ff)], local_sem.at[1]),
        pltpu.make_async_copy(up, ups.at[:, pl.ds(0, ff)], local_sem.at[2]),
        pltpu.make_async_copy(down, downs.at[pl.ds(0, ff)], local_sem.at[3]),
        pltpu.make_async_copy(pool_map, map_here, local_sem.at[4]),
        pltpu.make_async_copy(stream, stream_here, local_sem.at[5]),
    ]
    for at in (4, 0, 1, 2, 3, 5):
        own_copies[at].start()

    docs[...] = jnp.transpose(jnp.broadcast_to(docs_row[...].astype(F32), (128, rows)))
    pl.semaphore_wait(barrier, n_sp - 1 + 1 + n_chip - 1)

    right = ((sp + 1) % n_sp, tp)
    halo_copies = [
        remote(pool_in.at[pl.ds(rows - HALO, HALO)], halo, halo_ssem.at[0], halo_rsem.at[0], right),
        remote(docs.at[pl.ds(rows - HALO, HALO)], halo_docs, halo_ssem.at[1], halo_rsem.at[1], right),
    ]

    @pl.when(sp != n_sp - 1)
    def _():
        for c in halo_copies:
            c.start()

    @pl.when(sp == 0)
    def _():
        halo[...] = jnp.zeros_like(halo)
        halo_docs[...] = jnp.full_like(halo_docs, -1.0)


    def far_down(p, m):
        j = (n_chip - m) % n_chip
        return remote(
            down.at[:, wide(p)], downs.at[pl.ds(2 * j * ff, ff), wide(p)],
            w_ssem.at[m, p], w_rsem.at[2 * j, p], (sp, same(m)),
        )

    def near_down(p):
        return remote(
            down.at[:, wide(p)], downs.at[pl.ds(ff, ff), wide(p)],
            n_ssem.at[p], w_rsem.at[1, p], (sp, partner),
        )

    def forward_down(p, m):
        return remote(
            downs.at[pl.ds(2 * m * ff, ff), wide(p)],
            downs.at[pl.ds((2 * m + 1) * ff, ff), wide(p)],
            f_ssem.at[m, p], w_rsem.at[2 * m + 1, p], (sp, partner),
        )

    near_hidden = [
        remote(gate, gates.at[:, pl.ds(ff, ff)], g_ssem.at[0], g_rsem.at[0], (sp, partner)),
        remote(up, ups.at[:, pl.ds(ff, ff)], g_ssem.at[1], g_rsem.at[1], (sp, partner)),
    ]

    def send_down(*which):
        for p in which:
            for m in others:
                far_down(p, m).start()

    send_down(0, 1)

    window = jnp.left_shift(jnp.int32(2), tp)
    group_width = pool_in.shape[1]
    pooled = window_sums(
        jnp.zeros((HALO, group_width), F32), jnp.full((HALO, 128), -1.0, F32),
        pool_in[...].astype(F32), docs[...], window,
    )
    own_copies[4].wait()
    branch[...] = (
        jnp.dot(pooled, map_here[...], preferred_element_type=F32) * pool_scale[...]
    ).astype(BF16)
    own_copies[0].wait()

    def pair_owner(m):
        return (chip + m) % n_chip * 2 + other

    def pair_copy(m, c):
        return remote(
            pair_send.at[m, :, cols(c)], pair_recv.at[m, :, cols(c)],
            p_ssem.at[m, c], p_rsem.at[m, c], (sp, partner),
        )

    order = list(others) + [0]
    for c in range(chunks):
        partial[:, cols(c)] = jnp.dot(branch[...], outw[:, cols(c)], preferred_element_type=F32)
        for m in order:
            pair_send[m, :, cols(c)] = partial[owned(pair_owner(m)), cols(c)].astype(BF16)

            @pl.when(pair_owner(m) != 0)
            def _(m=m, c=c):
                pair_copy(m, c).start()

    @pl.when(sp != 0)
    def _():
        for c in halo_copies:
            c.wait_recv()

    head = window_sums(
        halo[...].astype(F32), halo_docs[...],
        pool_in[pl.ds(0, HALO), :].astype(F32), docs[pl.ds(0, HALO), :], window,
    )
    head = (jnp.dot(head, map_here[...], preferred_element_type=F32) * pool_scale[...]).astype(BF16)
    head = jnp.dot(head, outw[...], preferred_element_type=F32)
    partial[pl.ds(0, HALO), :] = head
    for m in order:
        @pl.when(pair_owner(m) == 0)
        def _(m=m):
            pair_send[m, pl.ds(0, HALO), :] = head.astype(BF16)
            for c in range(chunks):
                pair_copy(m, c).start()

    def far_copy(m, c):
        j = (n_chip - m) % n_chip
        return remote(
            far_send.at[m, :, cols(c)], far_recv.at[j, :, cols(c)],
            y_ssem.at[m, c], y_rsem.at[j, c], (sp, same(m)),
        )

    for m in others:
        for c in range(chunks):
            pair_copy(m, c).wait_recv()
            far_send[m, :, cols(c)] = (
                partial[owned(same(m)), cols(c)] + pair_recv[m, :, cols(c)].astype(F32)
            ).astype(BF16)
            far_copy(m, c).start()
    send_down(2)
    for c in near_hidden:
        c.start()
    for p in range(pieces):
        near_down(p).start()

    names = lax.broadcasted_iota(jnp.int32, (128, quarter), 0)
    above = (
        lax.broadcasted_iota(jnp.int32, (quarter, quarter), 0)
        < lax.broadcasted_iota(jnp.int32, (quarter, quarter), 1)
    ).astype(BF16)
    own_routes = routes[:, owned(tp)]

    def ranked(block_routes, first_slot, count):
        hots = [(block_routes[k : k + 1, :] == names).astype(F32) for k in range(top)]
        named = functools.reduce(lambda a, b: a + b, hots)
        before = jnp.dot(named.astype(BF16), above, preferred_element_type=F32)
        slot_names = lax.broadcasted_iota(jnp.int32, (count, quarter), 0) + first_slot
        places = []
        for k in range(top):
            rank = jnp.sum(hots[k] * before, axis=0, keepdims=True).astype(jnp.int32)
            places.append(
                (slot_names == block_routes[k : k + 1, :] * capacity + rank).astype(F32)
            )
        return places

    places = ranked(own_routes, 0, slots)
    spread = functools.reduce(lambda a, b: a + b, places).astype(BF16)
    sib_spread = {
        m: functools.reduce(
            lambda a, b: a + b,
            ranked(routes[:, owned(same(m))], team * half * capacity, half * capacity),
        ).astype(BF16)
        for m in others
    }
    picks = [jnp.transpose(p).astype(BF16) for p in places]
    scales = [
        jnp.transpose(jnp.broadcast_to(weights[k : k + 1, :], (128, quarter)))[:, :1]
        for k in range(top)
    ]

    everything = pl.ds(0, width)

    def outward(at, c=None):
        e = peer(at)
        columns = everything if c is None else cols(c)
        slot = c or 0
        return remote(
            dispatch.at[block(e), columns], arrived.at[pl.ds(at * capacity, capacity), columns],
            d_ssem.at[at, slot], d_rsem.at[at, slot], (e, tp),
        )

    def chunked(at):
        return at < span or half < at < half + span

    def gather_copy(m, c):
        j = (n_chip - m) % n_chip
        return remote(
            mixed.at[:, cols(c)], mixed_sib.at[j - 1, :, cols(c)],
            a_ssem.at[m, c], a_rsem.at[j, c], (sp, same(m)),
        )

    def gather(*which):
        for c in which:
            for m in others:
                gather_copy(m, c).start()

    def sib_outward(m, at):
        e = peer(at)
        return remote(
            dispatch_sib.at[m - 1, block(e - team * half)],
            crossed.at[m, pl.ds(at * capacity, capacity)],
            s_ssem.at[m, at], s_rsem.at[m, at], (e, tp),
        )

    own_copies[5].wait()
    for c in range(chunks):
        pair_copy(0, c).wait_recv()
        mine = partial[owned(tp), cols(c)] + pair_recv[0, :, cols(c)].astype(F32)
        for m in others:
            far_copy((n_chip - m) % n_chip, c).wait_recv()
            mine = mine + far_recv[m, :, cols(c)].astype(F32)
        mixed[:, cols(c)] = (stream_here[:, cols(c)].astype(F32) + mine).astype(BF16)
        dispatch[:, cols(c)] = jnp.dot(
            spread, mixed[:, cols(c)], preferred_element_type=F32
        ).astype(BF16)
        for at in range(n_sp):
            if chunked(at):
                outward(at, c).start()
    gather(0, 1, 2, 3)
    outer = member // span == team
    second, fourth = range(span, half), range(half + span, n_sp)

    @pl.when(outer)
    def _():
        for at in list(fourth) + list(second):
            outward(at).start()

    @pl.when(jnp.logical_not(outer))
    def _():
        for at in list(second) + list(fourth):
            outward(at).start()

    arrived[pl.ds(half * capacity, capacity), :] = dispatch[block(sp), :]

    size = span * capacity

    def places_of(g):
        return range(g * span, (g + 1) * span)

    def lines(g):
        return pl.ds(g * size, size)

    def gated(x):
        g = jnp.dot(x, gates[...], preferred_element_type=F32)
        u = jnp.dot(x, ups[...], preferred_element_type=F32)
        return (g / (1.0 + jnp.exp(-g)) * u).astype(BF16)

    def cross_copy(m, g):
        j = (n_chip - m) % n_chip
        return remote(
            crossed.at[0, lines(g)], crossed.at[j, lines(g)],
            c_ssem.at[m, g], c_rsem.at[j, g], (sp, same(m)),
        )

    def hidden_copy(j, g):
        m = (n_chip - j) % n_chip
        return remote(
            hidden_send.at[j - 1, lines(g)], hidden.at[lines(g), pl.ds(2 * m * ff, 2 * ff)],
            h_ssem.at[j, g], h_rsem.at[m, g], (sp, same(j)),
        )

    def normed(x):
        value = x.astype(F32)
        return (
            value * lax.rsqrt(jnp.mean(value * value, axis=1, keepdims=True) + EPS) * gain[...]
        ).astype(BF16)

    def normalize(g):
        for at in places_of(g):
            if chunked(at):
                for c in range(chunks):
                    outward(at, c).wait_recv()
            elif at != half:
                outward(at).wait_recv()
        crossed[0, lines(g), :] = normed(arrived[lines(g), :])
        if g < 2:
            for m in others:
                cross_copy(m, g).start()

    def sib_dispatch():
        for m in others:
            for c in range(chunks):
                gather_copy((n_chip - m) % n_chip, c).wait_recv()
                dispatch_sib[m - 1, :, cols(c)] = jnp.dot(
                    sib_spread[m], mixed_sib[m - 1, :, cols(c)], preferred_element_type=F32
                ).astype(BF16)
            for at in range(half + 1, n_sp):
                sib_outward(m, at).start()
            crossed[m, pl.ds(half * capacity, capacity), :] = dispatch_sib[m - 1, block(member), :]

    ready = []

    def own_hidden(g):
        if not ready:
            ready.append(True)
            for c in own_copies[1:3]:
                c.wait()
            for c in near_hidden:
                c.wait_recv()
        hidden[lines(g), pl.ds(0, 2 * ff)] = gated(crossed[0, lines(g), :])

    def far_hidden(g):
        for j in others:
            if g < 2:
                cross_copy((n_chip - j) % n_chip, g).wait_recv()
                x = crossed[j, lines(g), :]
            else:
                for at in places_of(g):
                    if at != half:
                        sib_outward(j, at).wait_recv()
                x = normed(crossed[j, lines(g), :])
            hidden_send[j - 1, lines(g), :] = gated(x)
            hidden_copy(j, g).start()

    held = set()

    def pass_down(*which):
        for p in which:
            for m in others:
                j = (n_chip - m) % n_chip
                far_down(p, j).wait_recv()
                forward_down(p, m).start()

    def homeward(at, p):
        e = peer(at)
        return remote(
            answers.at[pl.ds(at * capacity, capacity), wide(p)], returned.at[block(sp), wide(p)],
            r_ssem.at[at, p], r_rsem.at[at, p], (e, tp),
        )

    def answer(g, *which):
        if ("hidden", g) not in held:
            held.add(("hidden", g))
            for m in others:
                hidden_copy((n_chip - m) % n_chip, g).wait_recv()
        for p in which:
            if p not in held:
                if not held & set(range(pieces)):
                    own_copies[3].wait()
                held.add(p)
                near_down(p).wait_recv()
                for m in others:
                    forward_down(p, m).wait_recv()
            answers[lines(g), wide(p)] = jnp.dot(
                hidden[lines(g), :], downs[:, wide(p)], preferred_element_type=F32
            ).astype(BF16)
            for at in places_of(g):
                if at == half:
                    returned[block(sp), wide(p)] = answers[pl.ds(at * capacity, capacity), wide(p)]
                else:
                    homeward(at, p).start()

    normalize(2)
    own_hidden(2)
    normalize(0)
    send_down(3)
    own_hidden(0)
    sib_dispatch()
    pass_down(0, 1, 2)
    far_hidden(0)
    send_down(4)
    normalize(1)
    send_down(5)
    own_hidden(1)
    answer(0, 0, 1, 2)
    pass_down(3)
    answer(0, 3)
    normalize(3)
    own_hidden(3)
    far_hidden(2)
    far_hidden(1)
    far_hidden(3)
    send_down(6, 7)
    pass_down(4)
    answer(0, 4)
    answer(1, 0, 1, 2, 3, 4)
    pass_down(5)
    answer(0, 5)
    answer(1, 5)
    answer(2, 0, 1, 2, 3, 4, 5)
    pass_down(6)
    answer(0, 6)
    answer(1, 6)
    answer(3, 0, 1, 2, 3, 4, 5, 6)
    pass_down(7)
    answer(0, 7)
    answer(1, 7)
    answer(2, 6, 7)
    answer(3, 7)

    def out_copy(p):
        return pltpu.make_async_copy(
            out_here.at[:, wide(p)], out.at[:, wide(p)], out_sem.at[p]
        )

    @pl.when(sp != n_sp - 1)
    def _():
        for c in halo_copies:
            c.wait_send()

    for c in near_hidden:
        c.wait_send()
    for m in range(n_chip):
        for c in range(chunks):
            pair_copy(m, c).wait_send()
    for p in range(pieces):
        near_down(p).wait_send()
        for m in others:
            far_down(p, m).wait_send()
            forward_down(p, m).wait_send()
    for m in others:
        for c in range(chunks):
            far_copy(m, c).wait_send()
            gather_copy(m, c).wait_send()
        for g in range(4):
            if g < 2:
                cross_copy(m, g).wait_send()
            hidden_copy(m, g).wait_send()
        for at in range(half + 1, n_sp):
            sib_outward(m, at).wait_send()
    for at in range(n_sp):
        if at == half:
            continue
        if chunked(at):
            for c in range(chunks):
                outward(at, c).wait_send()
        else:
            outward(at).wait_send()

    for p in range(pieces):
        for at in range(n_sp):
            if at != half:
                homeward(at, p).wait_recv()
        result = mixed[:, wide(p)].astype(F32)
        for k in range(top):
            result = result + scales[k] * jnp.dot(
                picks[k], returned[:, wide(p)], preferred_element_type=F32
            )
        out_here[:, wide(p)] = result.astype(BF16)
        out_copy(p).start()

    for p in range(pieces):
        for at in range(n_sp):
            if at != half:
                homeward(at, p).wait_send()
        out_copy(p).wait()


def per_device(
    n_sp, n_tp,
    stream, pool_in, doc_ids, pool_map, pool_scale, out_weight, norm_gain, routes, route_weight,
    expert_gate, expert_up, expert_down,
):
    rows, group_width = pool_in.shape
    quarter, width = stream.shape
    top = routes.shape[1]
    ff = expert_gate.shape[2]
    capacity = max(2, 3 * top * quarter // (2 * n_sp))
    capacity = -(-capacity // 16) * 16
    slots = n_sp * capacity
    n_chip = n_tp // 2
    vmem = pl.BlockSpec(memory_space=pltpu.VMEM)
    hbm = pl.BlockSpec(memory_space=pl.ANY)
    dma = pltpu.SemaphoreType.DMA
    V = pltpu.VMEM
    branch_width = out_weight.shape[0]
    chunks = width // COLS
    pieces = width // PIECE
    return pl.pallas_call(
        functools.partial(kernel, n_sp, n_tp, quarter, capacity, top),
        out_shape=jax.ShapeDtypeStruct((quarter, width), BF16),
        in_specs=[hbm, vmem, vmem, hbm, vmem, hbm] + [vmem] * 3 + [hbm] * 3,
        out_specs=hbm,
        scratch_shapes=[
            V((width, 2 * ff), BF16),
            V((width, 2 * ff), BF16),
            V((n_tp * ff, width), BF16),
            V((branch_width, width), BF16),
            V((HALO, group_width), BF16),
            V((HALO, 128), F32),
            V((rows, branch_width), BF16),
            V((rows, width), F32),
            V((n_chip, quarter, width), BF16),
            V((n_chip, quarter, width), BF16),
            V((n_chip, quarter, width), BF16),
            V((n_chip, quarter, width), BF16),
            V((quarter, width), BF16),
            V((slots, width), BF16),
            V((slots, width), BF16),
            V((n_chip, slots, width), BF16),
            V((slots, n_tp * ff), BF16),
            V((n_chip - 1, slots, 2 * ff), BF16),
            V((slots, width), BF16),
            V((slots, width), BF16),
            V((n_chip - 1, quarter, width), BF16),
            V((n_chip - 1, n_sp // 2 * capacity, width), BF16),
            V((rows, 128), F32),
            V((group_width, branch_width), BF16),
            V((quarter, width), BF16),
            V((quarter, width), BF16),
            dma((6,)),
            dma((2,)),
            dma((2,)),
            dma((2,)),
            dma((2,)),
            dma((n_chip, pieces)),
            dma((n_tp, pieces)),
            dma((pieces,)),
            dma((n_chip, pieces)),
            dma((n_chip, chunks)),
            dma((n_chip, chunks)),
            dma((n_chip, chunks)),
            dma((n_chip, chunks)),
            dma((n_sp, chunks)),
            dma((n_sp, chunks)),
            dma((n_chip, 2)),
            dma((n_chip, 2)),
            dma((n_chip, 4)),
            dma((n_chip, 4)),
            dma((n_sp, pieces)),
            dma((n_sp, pieces)),
            dma((pieces,)),
            dma((n_chip, chunks)),
            dma((n_chip, chunks)),
            dma((n_chip, n_sp)),
            dma((n_chip, n_sp)),
        ],
        compiler_params=pltpu.CompilerParams(
            collective_id=0, has_side_effects=True, vmem_limit_bytes=60 * 1024 * 1024
        ),
    )(
        stream, pool_in, doc_ids[None, :], pool_map[0],
        pool_scale[None, :], out_weight, norm_gain[None, :], routes.T, route_weight.T,
        expert_gate[0], expert_up[0], expert_down[0],
    )


def solution(mesh):
    in_specs = (
        P(("sp", "tp"), None),
        P("sp", "tp"),
        P("sp"),
        P("tp", None, None),
        P("tp"),
        P("tp", None),
        P(),
        P("sp", None),
        P(("sp", "tp"), None),
        P("sp", None, "tp"),
        P("sp", None, "tp"),
        P("sp", "tp", None),
    )
    out_specs = P(("sp", "tp"), None)
    return jax.shard_map(
        functools.partial(per_device, mesh.shape["sp"], mesh.shape["tp"]),
        mesh=mesh, in_specs=in_specs, out_specs=out_specs, check_vma=False,
    )
```

```python
import functools

import jax
import jax.numpy as jnp
from jax import lax
from jax.experimental import pallas as pl
from jax.experimental.pallas import tpu as pltpu
from jax.sharding import PartitionSpec as P

HALO = 16
COLS = 512
PIECE = 256
EPS = 1e-06
MESH = pl.DeviceIdType.MESH
F32 = jnp.float32
BF16 = jnp.bfloat16


def flipped(index, mask):
    bit = 1
    while bit <= mask:
        if mask & bit:
            index = index + bit - 2 * bit * (index // bit % 2)
        bit *= 2
    return index


def window_sums(prior, prior_docs, own, own_docs, window):
    width = own.shape[1]
    ext_docs = jnp.concatenate([prior_docs, own_docs], axis=0)
    total = jnp.concatenate([prior, own], axis=0)
    counts = jnp.ones(ext_docs.shape, F32)
    step = 1
    while step < HALO:
        keep = (pltpu.roll(ext_docs, step, 0) == ext_docs) & (step < window)
        counts = counts + jnp.where(keep, pltpu.roll(counts, step, 0), 0.0)
        keep_wide = jnp.concatenate([keep.astype(F32)] * (width // 128), axis=1) > 0.5
        total = total + jnp.where(keep_wide, pltpu.roll(total, step, 0), 0.0)
        step *= 2
    counts_wide = jnp.concatenate([counts] * (width // 128), axis=1)
    return (total[HALO:] / counts_wide[HALO:] - own).astype(BF16)


def kernel(
    n_sp, n_tp, quarter, capacity, top,
    stream, pool_in, docs_row, pool_map, pool_scale, out_weight, gain, routes, weights,
    gate, up, down,
    out,
    gates, ups, downs, outw, halo, halo_docs, branch, partial, pair_send, pair_recv,
    far_send, far_recv, mixed, dispatch, arrived, crossed, hidden, hidden_send,
    answers, returned, mixed_sib, dispatch_sib, docs, map_here, stream_here, out_here,
    local_sem, halo_ssem, halo_rsem, g_ssem, g_rsem, w_ssem, w_rsem, n_ssem, f_ssem,
    p_ssem, p_rsem, y_ssem, y_rsem, d_ssem, d_rsem, c_ssem, c_rsem, h_ssem, h_rsem,
    r_ssem, r_rsem, out_sem, a_ssem, a_rsem, s_ssem, s_rsem,
):
    sp, tp = lax.axis_index("sp"), lax.axis_index("tp")
    n_chip = n_tp // 2
    chip, parity = tp // 2, tp % 2
    other = 1 - parity
    partner = chip * 2 + other
    rows = pool_in.shape[0]
    width = stream.shape[1]
    ff = gate.shape[1]
    slots = n_sp * capacity
    half = n_sp // 2
    team, member = sp // half, sp % half
    span = half // 2
    chunks = width // COLS
    pieces = width // PIECE
    others = range(1, n_chip)

    def same(m):
        return (chip + m) % n_chip * 2 + parity

    def remote(src, dst, ssem, rsem, to):
        return pltpu.make_async_remote_copy(
            src_ref=src, dst_ref=dst, send_sem=ssem, recv_sem=rsem,
            device_id=to, device_id_type=MESH,
        )

    def peer(at):
        if at < half:
            return (1 - team) * half + flipped(member, at)
        return team * half + flipped(member, at - half)

    def cols(c):
        return pl.ds(c * COLS, COLS)

    def wide(p):
        return pl.ds(p * PIECE, PIECE)

    def block(e):
        return pl.ds(pl.multiple_of(e * capacity, 16), capacity)

    def owned(q):
        return pl.ds(pl.multiple_of(q * quarter, quarter), quarter)

    barrier = pltpu.get_barrier_semaphore()
    for d in range(1, n_sp):
        pl.semaphore_signal(barrier, inc=1, device_id=((sp + d) % n_sp, tp), device_id_type=MESH)
    pl.semaphore_signal(barrier, inc=1, device_id=(sp, partner), device_id_type=MESH)
    for m in others:
        pl.semaphore_signal(barrier, inc=1, device_id=(sp, same(m)), device_id_type=MESH)

    own_copies = [
        pltpu.make_async_copy(out_weight, outw, local_sem.at[0]),
        pltpu.make_async_copy(gate, gates.at[:, pl.ds(0, ff)], local_sem.at[1]),
        pltpu.make_async_copy(up, ups.at[:, pl.ds(0, ff)], local_sem.at[2]),
        pltpu.make_async_copy(down, downs.at[pl.ds(0, ff)], local_sem.at[3]),
        pltpu.make_async_copy(pool_map, map_here, local_sem.at[4]),
        pltpu.make_async_copy(stream, stream_here, local_sem.at[5]),
    ]
    for at in (4, 0, 1, 2, 3, 5):
        own_copies[at].start()

    docs[...] = jnp.transpose(jnp.broadcast_to(docs_row[...].astype(F32), (128, rows)))
    pl.semaphore_wait(barrier, n_sp - 1 + 1 + n_chip - 1)

    right = ((sp + 1) % n_sp, tp)
    halo_copies = [
        remote(pool_in.at[pl.ds(rows - HALO, HALO)], halo, halo_ssem.at[0], halo_rsem.at[0], right),
        remote(docs.at[pl.ds(rows - HALO, HALO)], halo_docs, halo_ssem.at[1], halo_rsem.at[1], right),
    ]

    @pl.when(sp != n_sp - 1)
    def _():
        for c in halo_copies:
            c.start()

    @pl.when(sp == 0)
    def _():
        halo[...] = jnp.zeros_like(halo)
        halo_docs[...] = jnp.full_like(halo_docs, -1.0)


    def far_down(p, m):
        j = (n_chip - m) % n_chip
        return remote(
            down.at[:, wide(p)], downs.at[pl.ds(2 * j * ff, ff), wide(p)],
            w_ssem.at[m, p], w_rsem.at[2 * j, p], (sp, same(m)),
        )

    def near_down(p):
        return remote(
            down.at[:, wide(p)], downs.at[pl.ds(ff, ff), wide(p)],
            n_ssem.at[p], w_rsem.at[1, p], (sp, partner),
        )

    def forward_down(p, m):
        return remote(
            downs.at[pl.ds(2 * m * ff, ff), wide(p)],
            downs.at[pl.ds((2 * m + 1) * ff, ff), wide(p)],
            f_ssem.at[m, p], w_rsem.at[2 * m + 1, p], (sp, partner),
        )

    near_hidden = [
        remote(gate, gates.at[:, pl.ds(ff, ff)], g_ssem.at[0], g_rsem.at[0], (sp, partner)),
        remote(up, ups.at[:, pl.ds(ff, ff)], g_ssem.at[1], g_rsem.at[1], (sp, partner)),
    ]

    def send_down(*which):
        for p in which:
            for m in others:
                far_down(p, m).start()

    send_down(0)

    window = jnp.left_shift(jnp.int32(2), tp)
    group_width = pool_in.shape[1]
    pooled = window_sums(
        jnp.zeros((HALO, group_width), F32), jnp.full((HALO, 128), -1.0, F32),
        pool_in[...].astype(F32), docs[...], window,
    )
    own_copies[4].wait()
    branch[...] = (
        jnp.dot(pooled, map_here[...], preferred_element_type=F32) * pool_scale[...]
    ).astype(BF16)
    own_copies[0].wait()

    def pair_owner(m):
        return (chip + m) % n_chip * 2 + other

    def pair_copy(m, c):
        return remote(
            pair_send.at[m, :, cols(c)], pair_recv.at[m, :, cols(c)],
            p_ssem.at[m, c], p_rsem.at[m, c], (sp, partner),
        )

    order = list(others) + [0]
    for c in range(chunks):
        partial[:, cols(c)] = jnp.dot(branch[...], outw[:, cols(c)], preferred_element_type=F32)
        for m in order:
            pair_send[m, :, cols(c)] = partial[owned(pair_owner(m)), cols(c)].astype(BF16)

            @pl.when(pair_owner(m) != 0)
            def _(m=m, c=c):
                pair_copy(m, c).start()

    @pl.when(sp != 0)
    def _():
        for c in halo_copies:
            c.wait_recv()

    head = window_sums(
        halo[...].astype(F32), halo_docs[...],
        pool_in[pl.ds(0, HALO), :].astype(F32), docs[pl.ds(0, HALO), :], window,
    )
    head = (jnp.dot(head, map_here[...], preferred_element_type=F32) * pool_scale[...]).astype(BF16)
    head = jnp.dot(head, outw[...], preferred_element_type=F32)
    partial[pl.ds(0, HALO), :] = head
    for m in order:
        @pl.when(pair_owner(m) == 0)
        def _(m=m):
            pair_send[m, pl.ds(0, HALO), :] = head.astype(BF16)
            for c in range(chunks):
                pair_copy(m, c).start()

    def far_copy(m, c):
        j = (n_chip - m) % n_chip
        return remote(
            far_send.at[m, :, cols(c)], far_recv.at[j, :, cols(c)],
            y_ssem.at[m, c], y_rsem.at[j, c], (sp, same(m)),
        )

    for m in others:
        for c in range(chunks):
            pair_copy(m, c).wait_recv()
            far_send[m, :, cols(c)] = (
                partial[owned(same(m)), cols(c)] + pair_recv[m, :, cols(c)].astype(F32)
            ).astype(BF16)
            far_copy(m, c).start()
    send_down(1, 2)
    for c in near_hidden:
        c.start()
    for p in range(pieces):
        near_down(p).start()

    names = lax.broadcasted_iota(jnp.int32, (128, quarter), 0)
    above = (
        lax.broadcasted_iota(jnp.int32, (quarter, quarter), 0)
        < lax.broadcasted_iota(jnp.int32, (quarter, quarter), 1)
    ).astype(BF16)
    own_routes = routes[:, owned(tp)]

    def ranked(block_routes, first_slot, count):
        hots = [(block_routes[k : k + 1, :] == names).astype(F32) for k in range(top)]
        named = functools.reduce(lambda a, b: a + b, hots)
        before = jnp.dot(named.astype(BF16), above, preferred_element_type=F32)
        slot_names = lax.broadcasted_iota(jnp.int32, (count, quarter), 0) + first_slot
        places = []
        for k in range(top):
            rank = jnp.sum(hots[k] * before, axis=0, keepdims=True).astype(jnp.int32)
            places.append(
                (slot_names == block_routes[k : k + 1, :] * capacity + rank).astype(F32)
            )
        return places

    places = ranked(own_routes, 0, slots)
    spread = functools.reduce(lambda a, b: a + b, places).astype(BF16)
    sib_spread = {
        m: functools.reduce(
            lambda a, b: a + b,
            ranked(routes[:, owned(same(m))], team * half * capacity, half * capacity),
        ).astype(BF16)
        for m in others
    }
    picks = [jnp.transpose(p).astype(BF16) for p in places]
    scales = [
        jnp.transpose(jnp.broadcast_to(weights[k : k + 1, :], (128, quarter)))[:, :1]
        for k in range(top)
    ]

    everything = pl.ds(0, width)

    def outward(at, c=None):
        e = peer(at)
        columns = everything if c is None else cols(c)
        slot = c or 0
        return remote(
            dispatch.at[block(e), columns], arrived.at[pl.ds(at * capacity, capacity), columns],
            d_ssem.at[at, slot], d_rsem.at[at, slot], (e, tp),
        )

    def chunked(at):
        return at < span or half < at < half + span

    def gather_copy(m, c):
        j = (n_chip - m) % n_chip
        return remote(
            mixed.at[:, cols(c)], mixed_sib.at[j - 1, :, cols(c)],
            a_ssem.at[m, c], a_rsem.at[j, c], (sp, same(m)),
        )

    def gather(*which):
        for c in which:
            for m in others:
                gather_copy(m, c).start()

    def sib_outward(m, at):
        e = peer(at)
        return remote(
            dispatch_sib.at[m - 1, block(e - team * half)],
            crossed.at[m, pl.ds(at * capacity, capacity)],
            s_ssem.at[m, at], s_rsem.at[m, at], (e, tp),
        )

    own_copies[5].wait()
    for c in range(chunks):
        pair_copy(0, c).wait_recv()
        mine = partial[owned(tp), cols(c)] + pair_recv[0, :, cols(c)].astype(F32)
        for m in others:
            far_copy((n_chip - m) % n_chip, c).wait_recv()
            mine = mine + far_recv[m, :, cols(c)].astype(F32)
        mixed[:, cols(c)] = (stream_here[:, cols(c)].astype(F32) + mine).astype(BF16)
        dispatch[:, cols(c)] = jnp.dot(
            spread, mixed[:, cols(c)], preferred_element_type=F32
        ).astype(BF16)
        for at in range(n_sp):
            if chunked(at):
                outward(at, c).start()
    gather(0, 1, 2, 3)
    outer = member // span == team
    second, fourth = range(span, half), range(half + span, n_sp)

    @pl.when(outer)
    def _():
        for at in list(fourth) + list(second):
            outward(at).start()

    @pl.when(jnp.logical_not(outer))
    def _():
        for at in list(second) + list(fourth):
            outward(at).start()

    arrived[pl.ds(half * capacity, capacity), :] = dispatch[block(sp), :]

    size = span * capacity

    def places_of(g):
        return range(g * span, (g + 1) * span)

    def lines(g):
        return pl.ds(g * size, size)

    def gated(x):
        g = jnp.dot(x, gates[...], preferred_element_type=F32)
        u = jnp.dot(x, ups[...], preferred_element_type=F32)
        return (g / (1.0 + jnp.exp(-g)) * u).astype(BF16)

    def cross_copy(m, g):
        j = (n_chip - m) % n_chip
        return remote(
            crossed.at[0, lines(g)], crossed.at[j, lines(g)],
            c_ssem.at[m, g], c_rsem.at[j, g], (sp, same(m)),
        )

    def hidden_copy(j, g):
        m = (n_chip - j) % n_chip
        return remote(
            hidden_send.at[j - 1, lines(g)], hidden.at[lines(g), pl.ds(2 * m * ff, 2 * ff)],
            h_ssem.at[j, g], h_rsem.at[m, g], (sp, same(j)),
        )

    def normed(x):
        value = x.astype(F32)
        return (
            value * lax.rsqrt(jnp.mean(value * value, axis=1, keepdims=True) + EPS) * gain[...]
        ).astype(BF16)

    def normalize(g):
        for at in places_of(g):
            if chunked(at):
                for c in range(chunks):
                    outward(at, c).wait_recv()
            elif at != half:
                outward(at).wait_recv()
        crossed[0, lines(g), :] = normed(arrived[lines(g), :])
        if g < 2:
            for m in others:
                cross_copy(m, g).start()

    def sib_dispatch():
        for m in others:
            for c in range(chunks):
                gather_copy((n_chip - m) % n_chip, c).wait_recv()
                dispatch_sib[m - 1, :, cols(c)] = jnp.dot(
                    sib_spread[m], mixed_sib[m - 1, :, cols(c)], preferred_element_type=F32
                ).astype(BF16)
            for at in range(half + 1, n_sp):
                sib_outward(m, at).start()
            crossed[m, pl.ds(half * capacity, capacity), :] = dispatch_sib[m - 1, block(member), :]

    ready = []

    def own_hidden(g):
        if not ready:
            ready.append(True)
            for c in own_copies[1:3]:
                c.wait()
            for c in near_hidden:
                c.wait_recv()
        hidden[lines(g), pl.ds(0, 2 * ff)] = gated(crossed[0, lines(g), :])

    def far_hidden(g):
        for j in others:
            if g < 2:
                cross_copy((n_chip - j) % n_chip, g).wait_recv()
                x = crossed[j, lines(g), :]
            else:
                for at in places_of(g):
                    if at != half:
                        sib_outward(j, at).wait_recv()
                x = normed(crossed[j, lines(g), :])
            hidden_send[j - 1, lines(g), :] = gated(x)
            hidden_copy(j, g).start()

    held = set()

    def pass_down(*which):
        for p in which:
            for m in others:
                j = (n_chip - m) % n_chip
                far_down(p, j).wait_recv()
                forward_down(p, m).start()

    def homeward(at, p):
        e = peer(at)
        return remote(
            answers.at[pl.ds(at * capacity, capacity), wide(p)], returned.at[block(sp), wide(p)],
            r_ssem.at[at, p], r_rsem.at[at, p], (e, tp),
        )

    def answer(g, *which):
        if ("hidden", g) not in held:
            held.add(("hidden", g))
            for m in others:
                hidden_copy((n_chip - m) % n_chip, g).wait_recv()
        for p in which:
            if p not in held:
                if not held & set(range(pieces)):
                    own_copies[3].wait()
                held.add(p)
                near_down(p).wait_recv()
                for m in others:
                    forward_down(p, m).wait_recv()
            answers[lines(g), wide(p)] = jnp.dot(
                hidden[lines(g), :], downs[:, wide(p)], preferred_element_type=F32
            ).astype(BF16)
            for at in places_of(g):
                if at == half:
                    returned[block(sp), wide(p)] = answers[pl.ds(at * capacity, capacity), wide(p)]
                else:
                    homeward(at, p).start()

    normalize(2)
    own_hidden(2)
    normalize(0)
    send_down(3)
    own_hidden(0)
    sib_dispatch()
    pass_down(0, 1, 2)
    far_hidden(0)
    send_down(4)
    normalize(1)
    own_hidden(1)
    answer(0, 0, 1, 2)
    pass_down(3)
    answer(0, 3)
    far_hidden(2)
    pass_down(4)
    answer(0, 4)
    normalize(3)
    own_hidden(3)
    far_hidden(1)
    send_down(5, 6, 7)
    far_hidden(3)
    answer(1, 0, 1, 2, 3, 4)
    pass_down(5)
    answer(2, 0, 1, 2, 3, 4)
    answer(0, 5)
    answer(1, 5)
    pass_down(6)
    answer(2, 5)
    answer(3, 0, 1, 2)
    answer(0, 6)
    answer(1, 6)
    pass_down(7)
    answer(3, 3, 4, 5)
    answer(0, 7)
    answer(1, 7)
    answer(2, 6, 7)
    answer(3, 6, 7)

    def out_copy(p):
        return pltpu.make_async_copy(
            out_here.at[:, wide(p)], out.at[:, wide(p)], out_sem.at[p]
        )

    @pl.when(sp != n_sp - 1)
    def _():
        for c in halo_copies:
            c.wait_send()

    for c in near_hidden:
        c.wait_send()
    for m in range(n_chip):
        for c in range(chunks):
            pair_copy(m, c).wait_send()
    for p in range(pieces):
        near_down(p).wait_send()
        for m in others:
            far_down(p, m).wait_send()
            forward_down(p, m).wait_send()
    for m in others:
        for c in range(chunks):
            far_copy(m, c).wait_send()
            gather_copy(m, c).wait_send()
        for g in range(4):
            if g < 2:
                cross_copy(m, g).wait_send()
            hidden_copy(m, g).wait_send()
        for at in range(half + 1, n_sp):
            sib_outward(m, at).wait_send()
    for at in range(n_sp):
        if at == half:
            continue
        if chunked(at):
            for c in range(chunks):
                outward(at, c).wait_send()
        else:
            outward(at).wait_send()

    for p in range(pieces):
        for at in range(n_sp):
            if at != half:
                homeward(at, p).wait_recv()
        result = mixed[:, wide(p)].astype(F32)
        for k in range(top):
            result = result + scales[k] * jnp.dot(
                picks[k], returned[:, wide(p)], preferred_element_type=F32
            )
        out_here[:, wide(p)] = result.astype(BF16)
        out_copy(p).start()
        for at in range(n_sp):
            if at != half:
                homeward(at, p).wait_send()

    for p in range(pieces):
        out_copy(p).wait()


def per_device(
    n_sp, n_tp,
    stream, pool_in, doc_ids, pool_map, pool_scale, out_weight, norm_gain, routes, route_weight,
    expert_gate, expert_up, expert_down,
):
    rows, group_width = pool_in.shape
    quarter, width = stream.shape
    top = routes.shape[1]
    ff = expert_gate.shape[2]
    capacity = max(2, 3 * top * quarter // (2 * n_sp))
    capacity = -(-capacity // 16) * 16
    slots = n_sp * capacity
    n_chip = n_tp // 2
    vmem = pl.BlockSpec(memory_space=pltpu.VMEM)
    hbm = pl.BlockSpec(memory_space=pl.ANY)
    dma = pltpu.SemaphoreType.DMA
    V = pltpu.VMEM
    branch_width = out_weight.shape[0]
    chunks = width // COLS
    pieces = width // PIECE
    return pl.pallas_call(
        functools.partial(kernel, n_sp, n_tp, quarter, capacity, top),
        out_shape=jax.ShapeDtypeStruct((quarter, width), BF16),
        in_specs=[hbm, vmem, vmem, hbm, vmem, hbm] + [vmem] * 3 + [hbm] * 3,
        out_specs=hbm,
        scratch_shapes=[
            V((width, 2 * ff), BF16),
            V((width, 2 * ff), BF16),
            V((n_tp * ff, width), BF16),
            V((branch_width, width), BF16),
            V((HALO, group_width), BF16),
            V((HALO, 128), F32),
            V((rows, branch_width), BF16),
            V((rows, width), F32),
            V((n_chip, quarter, width), BF16),
            V((n_chip, quarter, width), BF16),
            V((n_chip, quarter, width), BF16),
            V((n_chip, quarter, width), BF16),
            V((quarter, width), BF16),
            V((slots, width), BF16),
            V((slots, width), BF16),
            V((n_chip, slots, width), BF16),
            V((slots, n_tp * ff), BF16),
            V((n_chip - 1, slots, 2 * ff), BF16),
            V((slots, width), BF16),
            V((slots, width), BF16),
            V((n_chip - 1, quarter, width), BF16),
            V((n_chip - 1, n_sp // 2 * capacity, width), BF16),
            V((rows, 128), F32),
            V((group_width, branch_width), BF16),
            V((quarter, width), BF16),
            V((quarter, width), BF16),
            dma((6,)),
            dma((2,)),
            dma((2,)),
            dma((2,)),
            dma((2,)),
            dma((n_chip, pieces)),
            dma((n_tp, pieces)),
            dma((pieces,)),
            dma((n_chip, pieces)),
            dma((n_chip, chunks)),
            dma((n_chip, chunks)),
            dma((n_chip, chunks)),
            dma((n_chip, chunks)),
            dma((n_sp, chunks)),
            dma((n_sp, chunks)),
            dma((n_chip, 2)),
            dma((n_chip, 2)),
            dma((n_chip, 4)),
            dma((n_chip, 4)),
            dma((n_sp, pieces)),
            dma((n_sp, pieces)),
            dma((pieces,)),
            dma((n_chip, chunks)),
            dma((n_chip, chunks)),
            dma((n_chip, n_sp)),
            dma((n_chip, n_sp)),
        ],
        compiler_params=pltpu.CompilerParams(
            collective_id=0, has_side_effects=True, vmem_limit_bytes=60 * 1024 * 1024
        ),
    )(
        stream, pool_in, doc_ids[None, :], pool_map[0],
        pool_scale[None, :], out_weight, norm_gain[None, :], routes.T, route_weight.T,
        expert_gate[0], expert_up[0], expert_down[0],
    )


def solution(mesh):
    in_specs = (
        P(("sp", "tp"), None),
        P("sp", "tp"),
        P("sp"),
        P("tp", None, None),
        P("tp"),
        P("tp", None),
        P(),
        P("sp", None),
        P(("sp", "tp"), None),
        P("sp", None, "tp"),
        P("sp", None, "tp"),
        P("sp", "tp", None),
    )
    out_specs = P(("sp", "tp"), None)
    return jax.shard_map(
        functools.partial(per_device, mesh.shape["sp"], mesh.shape["tp"]),
        mesh=mesh, in_specs=in_specs, out_specs=out_specs, check_vma=False,
    )
```
